32 devices in a mesh: sp: 16 (over z, y, x), tp: 2 (over core).
Axes of the slice: x: 2, y: 2, z: 4, core: 2. Of those that a mesh axis runs over, the one named last changes fastest.
Arguments:
- tokens: bfloat16 [3584, 2048], P('sp', 'tp'), may hold values from -6 to 6
- norm_gain: float32 [2048], replicated, may hold values from 0.1 to 1.9
- query_weight: bfloat16 [2048, 2048], P('sp', 'tp'), may hold values from -0.125 to 0.125
- key_weight: bfloat16 [2048, 1024], P('sp', 'tp'), may hold values from -0.125 to 0.125
- value_weight: bfloat16 [2048, 1024], P('sp', 'tp'), may hold values from -0.125 to 0.125
- glu_value_weight: bfloat16 [2048, 1536], P('sp', 'tp'), may hold values from -0.125 to 0.125
- glu_gate_weight: bfloat16 [2048, 1536], P('sp', 'tp'), may hold values from -0.125 to 0.125
- query_gain: float32 [64], replicated, may hold values from 1.2 to 1.6
- key_gain: float32 [64], replicated, may hold values from 1.1 to 1.4
- lambdas: float32 [16], P('tp'), may hold values from 0.3 to 0.8
- head_gain: float32 [128], replicated, may hold values from 0.1 to 1.9
- conv_weight: float32 [31, 1536], P(None, 'tp'), may hold values from -11 to 11
- channel_gain: float32 [1536], P('tp'), may hold values from 0.1 to 1.9
- attn_out_weight: bfloat16 [2048, 2048], P('sp', 'tp'), may hold values from -0.09375 to 0.09375
- conv_out_weight: bfloat16 [2048, 1536], P('sp', 'tp'), may hold values from -0.09375 to 0.09375
Outputs:
- mixed: bfloat16 [3584, 2048], P(('sp', 'tp'))
The draws below stay inside these ranges and needn't reach their ends.
All inputs are finite; a program needn't handle non-finite values.
Results may differ from the reference program's by a relative error of at most 0.014.
Values may be sent and summed in bfloat16 or wider, within the bound.
A program may use at most 128 MiB of HBM per device.

```python
import math
import jax
import jax.numpy as jnp
from jax import lax

D = 2048
HEADS = 16
KV_HEADS = 8
HEAD_DIM = 64
C_CH = 1536
CONV_W = 31
TOK_DEV = 224
SEQ = 3584


def draw_conv_weight(key, part):
    column = jnp.arange(C_CH, dtype=jnp.float32) / max(C_CH - 1, 1)
    base = jax.random.truncated_normal(key, -6.0, 6.0, (CONV_W, C_CH), jnp.float32)
    spread = jnp.exp(column * math.log(10.0))
    return base * spread * CONV_W ** (-0.5)


def shard_levels(key, extent, pieces, low, high):
    def one(position, blocks):
        draws = jax.random.uniform(jax.random.fold_in(jax.random.fold_in(key, 6), position), (blocks,), jnp.float32, low / len(pieces), high / len(pieces))
        return jnp.repeat(jnp.exp(draws), extent[position] // blocks).reshape((-1,) + (1,) * (len(extent) - position - 1))

    factor_of = one(*pieces[0])
    for cut in pieces[1:]:
        factor_of = factor_of * one(*cut)
    return factor_of


def centred(rng, shape, deviation, limit, cuts=(), held_as=jnp.bfloat16):
    drawn = jax.random.normal(rng, shape, jnp.float32) * deviation
    if len(cuts) > 0:
        drawn = shard_levels(rng, shape, cuts, -0.22, 0.18) * drawn
    return jnp.clip(drawn, min=-limit, max=limit).astype(held_as)


def setup_inputs(seed: int = 0) -> dict:
    splits = jax.random.split(jax.random.key(seed), 16)
    tokens = centred(splits[0], (SEQ, D), 1.0, 6.0, ((0, 16), (1, 2)))
    norm_gain = jnp.clip(1.0 + 0.18 * jax.random.normal(splits[1], (D,), jnp.float32), 0.1, 1.9)
    query_weight = centred(splits[2], (D, 2 * HEADS * HEAD_DIM), D ** -0.5, 0.125, ((0, 16), (1, 2)))
    key_weight = centred(splits[3], (D, 2 * KV_HEADS * HEAD_DIM), D ** -0.5, 0.125, ((0, 16), (1, 2)))
    value_weight = centred(splits[4], (D, 2 * KV_HEADS * HEAD_DIM), D ** -0.5, 0.125, ((0, 16), (1, 2)))
    glu_value_weight = centred(splits[5], (D, C_CH), D ** -0.5, 0.125, ((0, 16), (1, 2)))
    glu_gate_weight = centred(splits[6], (D, C_CH), D ** -0.5, 0.125, ((0, 16), (1, 2)))
    query_gain = jnp.clip(jax.random.uniform(splits[7], (HEAD_DIM,), jnp.float32, 1.2, 1.6), 1.2, 1.6)
    key_gain = jnp.clip(jax.random.uniform(splits[8], (HEAD_DIM,), jnp.float32, 1.1, 1.4), 1.1, 1.4)
    lambdas = jnp.clip(0.3 + 0.5 * jax.random.uniform(splits[9], (HEADS,), jnp.float32) ** shard_levels(splits[9], (HEADS,), ((0, 2),), -0.2, 0.2), 0.3, 0.8)
    head_gain = jnp.clip(1.0 + 0.18 * jax.random.normal(splits[10], (2 * HEAD_DIM,), jnp.float32), 0.1, 1.9)
    conv_weight = draw_conv_weight(jax.random.fold_in(splits[15], 71), 0)
    channel_gain = jnp.clip(1.0 + 0.18 * jax.random.normal(splits[12], (C_CH,), jnp.float32), 0.1, 1.9)
    attn_out_weight = centred(splits[13], (D, 2 * HEADS * HEAD_DIM), (2 * HEADS * HEAD_DIM + C_CH) ** -0.5, 0.09375, ((0, 16), (1, 2)))
    conv_out_weight = centred(splits[14], (D, C_CH), (2 * HEADS * HEAD_DIM + C_CH) ** -0.5, 0.09375, ((0, 16), (1, 2)))
    return {"tokens": tokens, "norm_gain": norm_gain, "query_weight": query_weight, "key_weight": key_weight, "value_weight": value_weight, "glu_value_weight": glu_value_weight, "glu_gate_weight": glu_gate_weight, "query_gain": query_gain, "key_gain": key_gain, "lambdas": lambdas, "head_gain": head_gain, "conv_weight": conv_weight, "channel_gain": channel_gain, "attn_out_weight": attn_out_weight, "conv_out_weight": conv_out_weight}


EPS = 1e-06
LAMBDA_INIT = 0.2

def rms_scale(values, gain):
    return values * lax.rsqrt(lax.optimization_barrier(jnp.mean(values * values, axis=-1, keepdims=True)) + EPS) * gain

def reference(tokens, norm_gain, query_weight, key_weight, value_weight, glu_value_weight, glu_gate_weight, query_gain, key_gain, lambdas, head_gain, conv_weight, channel_gain, attn_out_weight, conv_out_weight):
    seq_len = tokens.shape[0]
    normed = rms_scale(tokens.astype(jnp.float32), norm_gain).astype(jnp.bfloat16)
    queries = jnp.dot(normed, query_weight, preferred_element_type=jnp.float32).reshape(seq_len, HEADS, 2, HEAD_DIM)
    query_normed = rms_scale(queries, query_gain).astype(jnp.bfloat16)
    keys = jnp.dot(normed, key_weight, preferred_element_type=jnp.float32).reshape(seq_len, KV_HEADS, 2, HEAD_DIM)
    key_normed = rms_scale(keys, key_gain).astype(jnp.bfloat16)
    values = jnp.dot(normed, value_weight, preferred_element_type=jnp.float32).astype(jnp.bfloat16)
    values = values.reshape(seq_len, KV_HEADS, 2 * HEAD_DIM)
    group = HEADS // KV_HEADS
    key_all = jnp.repeat(key_normed, group, axis=1)
    value_all = jnp.repeat(values, group, axis=1)

    def one_head(inputs):
        head_query, head_key, head_value, weight_two = inputs
        key_float = head_key.astype(jnp.float32)
        value_float = head_value.astype(jnp.float32)

        def one_block(block_query):
            scores = jnp.einsum('bpd,npd->pbn', block_query.astype(jnp.float32), key_float) * HEAD_DIM ** (-0.5)
            expo = jnp.exp(scores - lax.optimization_barrier(jnp.max(scores, axis=-1, keepdims=True)))
            totals = lax.optimization_barrier(jnp.sum(expo, axis=-1))
            rounded = lax.optimization_barrier(expo.astype(jnp.bfloat16)).astype(jnp.float32)
            numer = jnp.einsum('pbn,nd->pbd', rounded, value_float)
            ratio = numer / totals[..., None]
            return ratio[0] - weight_two * ratio[1]
        blocks = lax.map(one_block, head_query.reshape(seq_len // TOK_DEV, TOK_DEV, 2, HEAD_DIM))
        return blocks.reshape(seq_len, 2 * HEAD_DIM)
    head_outs = lax.map(one_head, (query_normed.transpose(1, 0, 2, 3), key_all.transpose(1, 0, 2, 3), value_all.transpose(1, 0, 2), lambdas))
    att_rows = head_outs.transpose(1, 0, 2)
    att_out = (rms_scale(att_rows, head_gain) * (1.0 - LAMBDA_INIT)).astype(jnp.bfloat16)
    att_out = att_out.reshape(seq_len, HEADS * 2 * HEAD_DIM)
    glu_value = jnp.dot(normed, glu_value_weight, preferred_element_type=jnp.float32)
    glu_gate = jnp.dot(normed, glu_gate_weight, preferred_element_type=jnp.float32)
    glu_rows = (glu_value * jax.nn.sigmoid(glu_gate)).astype(jnp.bfloat16)
    reach = CONV_W // 2
    padded = jnp.pad(glu_rows.astype(jnp.float32), ((reach, reach), (0, 0)))
    conv_sum = jnp.zeros((seq_len, C_CH), jnp.float32)
    for offset in range(CONV_W):
        conv_sum = conv_sum + conv_weight[offset] * padded[offset:offset + seq_len]
    conv_out = jax.nn.silu(rms_scale(conv_sum, channel_gain)).astype(jnp.bfloat16)
    term = jnp.dot(att_out, attn_out_weight.T, preferred_element_type=jnp.float32)
    term = term + jnp.dot(conv_out, conv_out_weight.T, preferred_element_type=jnp.float32)
    return term.astype(jnp.bfloat16)
```

```python
import functools

import jax
import jax.numpy as jnp
from jax import lax
from jax.experimental import pallas as pl
from jax.experimental.pallas import tpu as pltpu
from jax.sharding import PartitionSpec as P

HEAD_DIM = 64
C_CH = 1536
CONV_W = 31


EPS = 1e-06
LAMBDA_INIT = 0.2


def with_halo(cells, sides, width):
    for axis, dim in sides:
        count = lax.axis_size(axis)
        ends = count - 1
        head = lax.slice_in_dim(cells, 0, width, axis=dim)
        tail = lax.slice_in_dim(cells, cells.shape[dim] - width, cells.shape[dim], axis=dim)
        cells = jnp.concatenate(
            [
                lax.ppermute(tail, axis, [(i, (i + 1) % count) for i in range(ends)]),
                cells,
                lax.ppermute(head, axis, [((i + 1) % count, i) for i in range(ends)]),
            ],
            axis=dim,
        )
    return cells


def rms_scale(values, gain):
    return values * lax.rsqrt(jnp.mean(values * values, axis=-1, keepdims=True) + EPS) * gain


def contract_last(left, right):
    return lax.dot_general(
        left, right, (((1,), (1,)), ((), ())), preferred_element_type=jnp.float32
    )


def local(
    tokens,
    norm_gain,
    query_weight,
    key_weight,
    value_weight,
    glu_value_weight,
    glu_gate_weight,
    query_gain,
    key_gain,
    lambdas,
    head_gain,
    conv_weight,
    channel_gain,
    attn_out_weight,
    conv_out_weight,
):
    gathered = lax.all_gather(tokens, "tp", axis=1, tiled=True).astype(jnp.float32)
    normed = rms_scale(gathered, norm_gain).astype(jnp.bfloat16)
    tok_rows, model_width = normed.shape
    pieces = (
        lax.all_gather(query_weight, "sp", axis=0, tiled=True),
        lax.all_gather(key_weight, "sp", axis=0, tiled=True),
        lax.all_gather(value_weight, "sp", axis=0, tiled=True),
        lax.all_gather(glu_value_weight, "sp", axis=0, tiled=True),
        lax.all_gather(glu_gate_weight, "sp", axis=0, tiled=True),
    )
    projected = tuple(
        (jnp.dot(normed, w_piece, preferred_element_type=jnp.float32) for w_piece in pieces)
    )
    q_heads = query_weight.shape[1] // (2 * HEAD_DIM)
    kv_heads = key_weight.shape[1] // (2 * HEAD_DIM)
    group = q_heads // kv_heads
    queries = projected[0].reshape(tok_rows, q_heads, 2, HEAD_DIM)
    query_normed = rms_scale(queries, query_gain).astype(jnp.bfloat16)
    query_blocks = query_normed.reshape(tok_rows, kv_heads, group, 2, HEAD_DIM).transpose(
        1, 2, 3, 0, 4
    )
    keys = projected[1].reshape(tok_rows, kv_heads, 2, HEAD_DIM)
    key_rows = (
        rms_scale(keys, key_gain).astype(jnp.bfloat16).reshape(tok_rows, kv_heads * 2 * HEAD_DIM)
    )
    value_rows = projected[2].astype(jnp.bfloat16)

    def attend_block(carry, key_block, value_block):
        run_max, run_sum, numer = carry
        key_count = key_block.shape[0]
        key_heads = key_block.reshape(key_count, kv_heads, 2, HEAD_DIM).transpose(1, 2, 0, 3)
        value_heads = value_block.reshape(key_count, kv_heads, 2 * HEAD_DIM).transpose(1, 0, 2)
        scores = jnp.einsum(
            "kgprd,kpnd->kgprn", query_blocks, key_heads, preferred_element_type=jnp.float32
        ) * HEAD_DIM ** (-0.5)
        new_max = jnp.maximum(run_max, jnp.max(scores, axis=-1))
        expo = jnp.exp(scores - new_max[..., None])
        factor = jnp.exp(run_max - new_max)
        run_sum = run_sum * factor + jnp.sum(expo, axis=-1)
        numer = numer * factor[..., None] + jnp.einsum(
            "kgprn,knd->kgprd",
            expo.astype(jnp.bfloat16),
            value_heads,
            preferred_element_type=jnp.float32,
        )
        return (new_max, run_sum, numer)

    start_carry = (
        jnp.full((kv_heads, group, 2, tok_rows), -jnp.inf, jnp.float32),
        jnp.zeros((kv_heads, group, 2, tok_rows), jnp.float32),
        jnp.zeros((kv_heads, group, 2, tok_rows, 2 * HEAD_DIM), jnp.float32),
    )
    carry = start_carry
    pieces = (
        lax.all_gather(key_rows, "sp", axis=0, tiled=True),
        lax.all_gather(value_rows, "sp", axis=0, tiled=True),
    )
    key_count = pieces[0].shape[0]
    step_rows = key_count
    while step_rows > 1024 and step_rows % 2 == 0:
        step_rows = step_rows // 2
    turn_count = key_count // step_rows
    key_steps = pieces[0].reshape(turn_count, step_rows, pieces[0].shape[1])
    value_steps = pieces[1].reshape(turn_count, step_rows, pieces[1].shape[1])

    def one_turn(inner, both):
        return (attend_block(inner, both[0], both[1]), None)

    carry, unused = lax.scan(one_turn, carry, (key_steps, value_steps))
    run_max, run_sum, numer = carry
    ratio = numer / run_sum[..., None]
    weight_two = lambdas.reshape(kv_heads, group, 1, 1)
    difference = ratio[:, :, 0] - weight_two * ratio[:, :, 1]
    att_rows = difference.transpose(2, 0, 1, 3).reshape(tok_rows, q_heads, 2 * HEAD_DIM)
    att_normed = (rms_scale(att_rows, head_gain) * (1.0 - LAMBDA_INIT)).astype(jnp.bfloat16)
    att_out = att_normed.reshape(tok_rows, q_heads * 2 * HEAD_DIM)
    glu_rows = (projected[3] * jax.nn.sigmoid(projected[4])).astype(jnp.bfloat16)
    padded = with_halo(glu_rows, (("sp", 0),), CONV_W // 2)
    conv_sum = jnp.zeros((tok_rows, glu_rows.shape[1]), jnp.float32)
    for offset in range(CONV_W):
        conv_sum = conv_sum + conv_weight[offset] * padded[offset : offset + tok_rows].astype(
            jnp.float32
        )
    squares = lax.psum(jnp.sum(conv_sum * conv_sum, axis=1), "tp")
    scaled = conv_sum * lax.rsqrt(squares / C_CH + EPS)[:, None] * channel_gain
    conv_out = jax.nn.silu(scaled).astype(jnp.bfloat16)
    pieces = (
        lax.all_gather(attn_out_weight, "sp", axis=0, tiled=True),
        lax.all_gather(conv_out_weight, "sp", axis=0, tiled=True),
    )
    partial_term = contract_last(att_out, pieces[0]) + contract_last(conv_out, pieces[1])
    return lax.psum_scatter(
        partial_term.astype(jnp.bfloat16), "tp", scatter_dimension=0, tiled=True
    )


PLANE = 4
RING = 4
LOG2E = 1.4426950408889634


def where_am_i():
    me = lax.axis_index("sp")
    core = lax.axis_index("tp")
    group = me // PLANE
    spot = me % PLANE
    along_y = spot // 2
    along_x = spot % 2
    x_peer = group * PLANE + along_y * 2 + (1 - along_x)
    y_peer = group * PLANE + (1 - along_y) * 2 + along_x
    diagonal = group * PLANE + (1 - along_y) * 2 + (1 - along_x)
    right = ((group + 1) % RING) * PLANE + spot
    left = ((group + RING - 1) % RING) * PLANE + spot
    return core, group, spot, x_peer, y_peer, diagonal, right, left


def at(sp, tp):
    return {"sp": sp, "tp": tp}


def greet(peers):
    barrier = pltpu.get_barrier_semaphore()
    for peer in peers:
        pl.semaphore_signal(
            barrier, inc=1, device_id=peer, device_id_type=pl.DeviceIdType.MESH
        )
    pl.semaphore_wait(barrier, len(peers))


def send(src, dst, send_sem, recv_sem, peer):
    copy = pltpu.make_async_remote_copy(
        src_ref=src,
        dst_ref=dst,
        send_sem=send_sem,
        recv_sem=recv_sem,
        device_id=peer,
        device_id_type=pl.DeviceIdType.MESH,
    )
    copy.start()
    return copy


def gather_kernel(w_ref, t_ref, wout, tout, own_sem, ws, wr, zs, zr, ts, tr, ps, pr):
    core, group, spot, x_peer, y_peer, diagonal, right, left = where_am_i()
    other = 1 - core
    me = group * PLANE + spot
    greet(
        [
            at(x_peer, core),
            at(y_peer, core),
            at(diagonal, core),
            at(right, core),
            at(left, core),
            at(me, other),
        ]
    )
    mine_w = pltpu.make_async_copy(w_ref.at[spot], wout.at[group, spot], own_sem.at[0])
    mine_w.start()
    mine_t = pltpu.make_async_copy(t_ref, tout.at[core, spot], own_sem.at[1])
    mine_t.start()
    first = []
    for slot, peer in enumerate((x_peer, y_peer, diagonal)):
        first.append(
            send(
                w_ref.at[peer % PLANE],
                wout.at[group, spot],
                ws.at[slot],
                wr.at[slot],
                at(peer, core),
            )
        )
    tok = [
        send(t_ref, tout.at[core, spot], ts.at[0], tr.at[0], at(x_peer, core)),
        send(t_ref, tout.at[core, spot], ts.at[1], tr.at[1], at(y_peer, core)),
    ]
    part = [send(t_ref, tout.at[core, spot], ps.at[0], pr.at[0], at(me, other))]
    mine_w.wait()
    for copy in first:
        copy.wait_recv()
    ring = [
        send(wout.at[group], wout.at[group], zs.at[0], zr.at[0], at(right, core)),
        send(wout.at[group], wout.at[group], zs.at[1], zr.at[1], at(left, core)),
    ]
    half = t_ref.shape[0] // 2
    from_x = x_peer % PLANE
    from_y = y_peer % PLANE
    from_d = diagonal % PLANE
    tok[0].wait_recv()
    block = tout.at[core, from_x]
    piece = tout.at[core, from_x, pl.ds(0, half)]
    tok.append(send(piece, piece, ts.at[2], tr.at[2], at(y_peer, core)))
    part.append(send(block, block, ps.at[1], pr.at[1], at(me, other)))
    tok[1].wait_recv()
    block = tout.at[core, from_y]
    piece = tout.at[core, from_y, pl.ds(half, half)]
    tok.append(send(piece, piece, ts.at[3], tr.at[3], at(x_peer, core)))
    part.append(send(block, block, ps.at[2], pr.at[2], at(me, other)))
    tok[2].wait_recv()
    tok[3].wait_recv()
    block = tout.at[core, from_d]
    part.append(send(block, block, ps.at[3], pr.at[3], at(me, other)))
    cut = PLANE // 2
    from_left = left // PLANE
    from_right = right // PLANE
    ring[0].wait_recv()
    piece = wout.at[from_left, pl.ds(0, cut)]
    ring.append(send(piece, piece, zs.at[2], zr.at[2], at(right, core)))
    ring[1].wait_recv()
    piece = wout.at[from_right, pl.ds(cut, cut)]
    ring.append(send(piece, piece, zs.at[3], zr.at[3], at(left, core)))
    for copy in part:
        copy.wait_recv()
    ring[2].wait_recv()
    ring[3].wait_recv()
    for copy in first + tok + part + ring:
        copy.wait_send()
    mine_t.wait()


def keys_kernel(kv_ref, edge_ref, kv_out, edge_out, own_sem, zs, zr, es, er):
    core, group, spot, x_peer, y_peer, diagonal, right, left = where_am_i()
    greet([at(right, core), at(left, core)])
    mine = pltpu.make_async_copy(kv_ref, kv_out.at[group], own_sem.at[0])
    mine.start()
    edges = [
        send(edge_ref.at[1], edge_out.at[0], es.at[0], er.at[0], at(right, core)),
        send(edge_ref.at[0], edge_out.at[1], es.at[1], er.at[1], at(left, core)),
    ]
    ring = [
        send(kv_ref, kv_out.at[group], zs.at[0], zr.at[0], at(right, core)),
        send(kv_ref, kv_out.at[group], zs.at[1], zr.at[1], at(left, core)),
    ]
    half = kv_ref.shape[0] // 2
    ring[0].wait_recv()
    piece = kv_out.at[left // PLANE, pl.ds(0, half)]
    ring.append(send(piece, piece, zs.at[2], zr.at[2], at(right, core)))
    ring[1].wait_recv()
    piece = kv_out.at[right // PLANE, pl.ds(half, half)]
    ring.append(send(piece, piece, zs.at[3], zr.at[3], at(left, core)))
    mine.wait()
    ring[2].wait_recv()
    ring[3].wait_recv()
    for copy in edges:
        copy.wait()
    for copy in ring:
        copy.wait_send()


def squares_kernel(sq_ref, out_ref, own_sem, ss, sr):
    core, group, spot, x_peer, y_peer, diagonal, right, left = where_am_i()
    me = group * PLANE + spot
    other = 1 - core
    peers = [at(me, other)]
    for chip in (x_peer, y_peer, diagonal):
        peers.append(at(chip, core))
        peers.append(at(chip, other))
    greet(peers)
    mine = pltpu.make_async_copy(sq_ref, out_ref.at[spot * 2 + core], own_sem.at[0])
    mine.start()
    copies = [
        send(sq_ref, out_ref.at[spot * 2 + core], ss.at[i], sr.at[i], peer)
        for i, peer in enumerate(peers)
    ]
    mine.wait()
    for copy in copies:
        copy.wait()


def sum_kernel(p_ref, o_ref, near, mid, far, ns, nr, fs, fr):
    core, group, spot, x_peer, y_peer, diagonal, right, left = where_am_i()
    me = group * PLANE + spot
    other = 1 - core
    chips = (diagonal, x_peer, y_peer, me)
    greet([at(me, other)] + [at(chip, core) for chip in chips[:3]])
    inner = [
        send(
            p_ref.at[chip % PLANE, other],
            near.at[slot],
            ns.at[slot],
            nr.at[slot],
            at(me, other),
        )
        for slot, chip in enumerate(chips)
    ]
    outer = []
    for slot, chip in enumerate(chips):
        inner[slot].wait_recv()
        total = p_ref[chip % PLANE, core].astype(jnp.float32) + near[slot].astype(jnp.float32)
        if slot < 3:
            mid[slot] = total.astype(jnp.bfloat16)
            outer.append(
                send(mid.at[slot], far.at[slot], fs.at[slot], fr.at[slot], at(chip, core))
            )
    for slot in range(3):
        outer[slot].wait_recv()
        total = total + far[slot].astype(jnp.float32)
    o_ref[...] = total.astype(o_ref.dtype)
    for copy in inner + outer:
        copy.wait_send()


def attend_kernel(lam_ref, gain_ref, q_ref, kv_ref, o_ref, *, step):
    width = 2 * HEAD_DIM
    tall = q_ref.shape[2]
    ratios = []
    for pair in range(2):
        query = q_ref[0, pair]
        numer = jnp.zeros((tall, width), jnp.float32)
        sums = jnp.zeros((tall, width), jnp.float32)
        for start in range(0, kv_ref.shape[0], step):
            scores = contract_last(query, kv_ref[start : start + step, :width])
            expo = jnp.exp2(scores * (LOG2E * HEAD_DIM ** (-0.5)))
            for lane in range(0, step, width):
                sums = sums + expo[:, lane : lane + width]
            numer = numer + jnp.dot(
                expo.astype(jnp.bfloat16),
                kv_ref[start : start + step, width:],
                preferred_element_type=jnp.float32,
            )
        ratios.append(numer / jnp.sum(sums, axis=1, keepdims=True))
    rows = ratios[0] - lam_ref[pl.program_id(0)] * ratios[1]
    o_ref[...] = (rms_scale(rows, gain_ref[...]) * (1.0 - LAMBDA_INIT)).astype(o_ref.dtype)


VMEM = pl.BlockSpec(memory_space=pltpu.VMEM)
DMA = pltpu.SemaphoreType.DMA


def exchange(kernel, number, shapes, scratch, *operands):
    return pl.pallas_call(
        kernel,
        out_shape=shapes,
        in_specs=[VMEM] * len(operands),
        out_specs=jax.tree.map(lambda _: VMEM, shapes),
        scratch_shapes=scratch,
        compiler_params=pltpu.CompilerParams(
            collective_id=number, has_side_effects=True, vmem_limit_bytes=48 * 2**20
        ),
        name=kernel.__name__,
    )(*operands)


def grouped(
    tokens,
    norm_gain,
    query_weight,
    key_weight,
    value_weight,
    glu_value_weight,
    glu_gate_weight,
    query_gain,
    key_gain,
    lambdas,
    head_gain,
    conv_weight,
    channel_gain,
    attn_out_weight,
    conv_out_weight,
):
    bf16, f32 = jnp.bfloat16, jnp.float32
    shape = jax.ShapeDtypeStruct
    me = lax.axis_index("sp")
    group, spot = me // PLANE, me % PLANE
    weights = (
        query_weight,
        key_weight,
        value_weight,
        attn_out_weight,
        glu_value_weight,
        glu_gate_weight,
        conv_out_weight,
    )
    depth = query_weight.shape[0]
    widths = [w.shape[1] // PLANE for w in weights]
    packed = jnp.concatenate(
        [w.reshape(depth, PLANE, n) for w, n in zip(weights, widths)], axis=2
    ).transpose(1, 0, 2)
    tok_rows, half_width = tokens.shape
    w_all, t_all = exchange(
        gather_kernel,
        0,
        (
            shape((RING, PLANE, depth, packed.shape[2]), bf16),
            shape((2, PLANE, tok_rows, half_width), bf16),
        ),
        [DMA((2,)), DMA((3,)), DMA((3,))] + [DMA((4,))] * 6,
        packed,
        tokens,
    )
    w_all = w_all.reshape(RING * PLANE * depth, packed.shape[2])
    rows = PLANE * tok_rows
    gathered = jnp.concatenate(
        [t_all[0].reshape(rows, half_width), t_all[1].reshape(rows, half_width)], axis=1
    ).astype(f32)
    normed = rms_scale(gathered, norm_gain).astype(bf16)
    ends = [sum(widths[:i]) for i in range(len(widths) + 1)]

    def project(first, last):
        return jnp.dot(
            normed, w_all[:, ends[first] : ends[last]], preferred_element_type=f32
        )

    width = 2 * HEAD_DIM
    q_heads = widths[0] // width
    qkv = project(0, 3)
    queries = qkv[:, : ends[1]].reshape(rows, q_heads, 2, HEAD_DIM)
    queries = rms_scale(queries, query_gain).astype(bf16)
    low = jnp.pad(queries[:, :, 0], ((0, 0), (0, 0), (0, HEAD_DIM)))
    high = jnp.pad(queries[:, :, 1], ((0, 0), (0, 0), (HEAD_DIM, 0)))
    queries = jnp.stack([low, high], axis=0).transpose(2, 0, 1, 3)
    keys = qkv[:, ends[1] : ends[2]].reshape(rows, 2, HEAD_DIM)
    keys = rms_scale(keys, key_gain).astype(bf16).reshape(rows, width)
    kv = jnp.concatenate([keys, qkv[:, ends[2] : ends[3]].astype(bf16)], axis=1)
    glu = project(4, 6)
    channels = widths[4]
    glu_rows = (glu[:, :channels] * jax.nn.sigmoid(glu[:, channels:])).astype(bf16)
    reach = CONV_W // 2
    border = 16
    edges = jnp.stack([glu_rows[:border], glu_rows[rows - border :]])
    kv_all, halo = exchange(
        keys_kernel,
        1,
        (shape((RING, rows, 2 * width), bf16), shape(edges.shape, bf16)),
        [DMA((1,)), DMA((4,)), DMA((4,)), DMA((2,)), DMA((2,))],
        kv,
        edges,
    )
    before = jnp.where(group > 0, halo[0], 0)[border - reach :]
    after = jnp.where(group < RING - 1, halo[1], 0)[:reach]
    padded = jnp.concatenate([before, glu_rows, after], axis=0).astype(f32)
    taps = lax.dynamic_slice_in_dim(conv_weight, spot * channels, channels, axis=1)
    gains = lax.dynamic_slice_in_dim(channel_gain, spot * channels, channels, axis=0)
    conv_sum = jnp.zeros((rows, channels), f32)
    for offset in range(CONV_W):
        conv_sum = conv_sum + taps[offset] * padded[offset : offset + rows]
    squares = jnp.sum(conv_sum * conv_sum, axis=1).reshape(rows // 128, 128)
    squares = jnp.pad(squares, ((0, -squares.shape[0] % 8), (0, 0)))
    shared = exchange(
        squares_kernel,
        2,
        shape((2 * PLANE,) + squares.shape, f32),
        [DMA((1,)), DMA((7,)), DMA((7,))],
        squares,
    )
    squares = jnp.sum(shared, axis=0).reshape(-1)[:rows]
    scaled = conv_sum * lax.rsqrt(squares / C_CH + EPS)[:, None] * gains
    conv_out = jax.nn.silu(scaled).astype(bf16)

    lam = lax.dynamic_slice_in_dim(lambdas, spot * q_heads, q_heads, axis=0)
    total = RING * rows
    tall = rows // 2
    att_out = pl.pallas_call(
        functools.partial(attend_kernel, step=512),
        out_shape=shape((rows, q_heads * width), bf16),
        grid=(q_heads, 2),
        in_specs=[
            pl.BlockSpec(memory_space=pltpu.SMEM),
            pl.BlockSpec((1, width), lambda h, t: (0, 0)),
            pl.BlockSpec((1, 2, tall, width), lambda h, t: (h, 0, t, 0)),
            pl.BlockSpec((total, 2 * width), lambda h, t: (0, 0)),
        ],
        out_specs=pl.BlockSpec((tall, width), lambda h, t: (t, h)),
        compiler_params=pltpu.CompilerParams(vmem_limit_bytes=48 * 2**20),
        name="attend",
    )(lam, head_gain.reshape(1, width), queries, kv_all.reshape(total, 2 * width))

    mixed = contract_last(att_out, w_all[:, ends[3] : ends[4]]) + contract_last(
        conv_out, w_all[:, ends[6] : ends[7]]
    )
    mixed = mixed.astype(bf16).reshape(PLANE, 2, tok_rows // 2, mixed.shape[1])
    block = mixed.shape[2:]
    return exchange(
        sum_kernel,
        3,
        shape(block, bf16),
        [
            pltpu.VMEM((4,) + block, bf16),
            pltpu.VMEM((3,) + block, bf16),
            pltpu.VMEM((3,) + block, bf16),
            DMA((4,)),
            DMA((4,)),
            DMA((3,)),
            DMA((3,)),
        ],
        mixed,
    )


def body_for(mesh):
    if mesh.shape["sp"] == RING * PLANE and mesh.shape["tp"] == 2:
        return grouped
    return local


def solution(mesh):
    return jax.shard_map(
        body_for(mesh),
        mesh=mesh,
        in_specs=(
            P("sp", "tp"),
            P(),
            P("sp", "tp"),
            P("sp", "tp"),
            P("sp", "tp"),
            P("sp", "tp"),
            P("sp", "tp"),
            P(),
            P(),
            P("tp"),
            P(),
            P(None, "tp"),
            P("tp"),
            P("sp", "tp"),
            P("sp", "tp"),
        ),
        out_specs=P(("sp", "tp"), None),
        check_vma=False,
    )
```

```python
import jax
import jax.numpy as jnp
from jax import lax
from jax.experimental import pallas as pl
from jax.experimental.pallas import tpu as pltpu
from jax.sharding import PartitionSpec as P

HEAD_DIM = 64
C_CH = 1536
CONV_W = 31


EPS = 1e-06
LAMBDA_INIT = 0.2


def with_halo(cells, sides, width):
    for axis, dim in sides:
        count = lax.axis_size(axis)
        ends = count - 1
        head = lax.slice_in_dim(cells, 0, width, axis=dim)
        tail = lax.slice_in_dim(cells, cells.shape[dim] - width, cells.shape[dim], axis=dim)
        cells = jnp.concatenate(
            [
                lax.ppermute(tail, axis, [(i, (i + 1) % count) for i in range(ends)]),
                cells,
                lax.ppermute(head, axis, [((i + 1) % count, i) for i in range(ends)]),
            ],
            axis=dim,
        )
    return cells


def rms_scale(values, gain):
    return values * lax.rsqrt(jnp.mean(values * values, axis=-1, keepdims=True) + EPS) * gain


def contract_last(left, right):
    return lax.dot_general(
        left, right, (((1,), (1,)), ((), ())), preferred_element_type=jnp.float32
    )


def local(
    tokens,
    norm_gain,
    query_weight,
    key_weight,
    value_weight,
    glu_value_weight,
    glu_gate_weight,
    query_gain,
    key_gain,
    lambdas,
    head_gain,
    conv_weight,
    channel_gain,
    attn_out_weight,
    conv_out_weight,
):
    gathered = lax.all_gather(tokens, "tp", axis=1, tiled=True).astype(jnp.float32)
    normed = rms_scale(gathered, norm_gain).astype(jnp.bfloat16)
    tok_rows, model_width = normed.shape
    pieces = (
        lax.all_gather(query_weight, "sp", axis=0, tiled=True),
        lax.all_gather(key_weight, "sp", axis=0, tiled=True),
        lax.all_gather(value_weight, "sp", axis=0, tiled=True),
        lax.all_gather(glu_value_weight, "sp", axis=0, tiled=True),
        lax.all_gather(glu_gate_weight, "sp", axis=0, tiled=True),
    )
    projected = tuple(
        (jnp.dot(normed, w_piece, preferred_element_type=jnp.float32) for w_piece in pieces)
    )
    q_heads = query_weight.shape[1] // (2 * HEAD_DIM)
    kv_heads = key_weight.shape[1] // (2 * HEAD_DIM)
    group = q_heads // kv_heads
    queries = projected[0].reshape(tok_rows, q_heads, 2, HEAD_DIM)
    query_normed = rms_scale(queries, query_gain).astype(jnp.bfloat16)
    query_blocks = query_normed.reshape(tok_rows, kv_heads, group, 2, HEAD_DIM).transpose(
        1, 2, 3, 0, 4
    )
    keys = projected[1].reshape(tok_rows, kv_heads, 2, HEAD_DIM)
    key_rows = (
        rms_scale(keys, key_gain).astype(jnp.bfloat16).reshape(tok_rows, kv_heads * 2 * HEAD_DIM)
    )
    value_rows = projected[2].astype(jnp.bfloat16)

    def attend_block(carry, key_block, value_block):
        run_max, run_sum, numer = carry
        key_count = key_block.shape[0]
        key_heads = key_block.reshape(key_count, kv_heads, 2, HEAD_DIM).transpose(1, 2, 0, 3)
        value_heads = value_block.reshape(key_count, kv_heads, 2 * HEAD_DIM).transpose(1, 0, 2)
        scores = jnp.einsum(
            "kgprd,kpnd->kgprn", query_blocks, key_heads, preferred_element_type=jnp.float32
        ) * HEAD_DIM ** (-0.5)
        new_max = jnp.maximum(run_max, jnp.max(scores, axis=-1))
        expo = jnp.exp(scores - new_max[..., None])
        factor = jnp.exp(run_max - new_max)
        run_sum = run_sum * factor + jnp.sum(expo, axis=-1)
        numer = numer * factor[..., None] + jnp.einsum(
            "kgprn,knd->kgprd",
            expo.astype(jnp.bfloat16),
            value_heads,
            preferred_element_type=jnp.float32,
        )
        return (new_max, run_sum, numer)

    start_carry = (
        jnp.full((kv_heads, group, 2, tok_rows), -jnp.inf, jnp.float32),
        jnp.zeros((kv_heads, group, 2, tok_rows), jnp.float32),
        jnp.zeros((kv_heads, group, 2, tok_rows, 2 * HEAD_DIM), jnp.float32),
    )
    carry = start_carry
    pieces = (
        lax.all_gather(key_rows, "sp", axis=0, tiled=True),
        lax.all_gather(value_rows, "sp", axis=0, tiled=True),
    )
    key_count = pieces[0].shape[0]
    step_rows = key_count
    while step_rows > 1024 and step_rows % 2 == 0:
        step_rows = step_rows // 2
    turn_count = key_count // step_rows
    key_steps = pieces[0].reshape(turn_count, step_rows, pieces[0].shape[1])
    value_steps = pieces[1].reshape(turn_count, step_rows, pieces[1].shape[1])

    def one_turn(inner, both):
        return (attend_block(inner, both[0], both[1]), None)

    carry, unused = lax.scan(one_turn, carry, (key_steps, value_steps))
    run_max, run_sum, numer = carry
    ratio = numer / run_sum[..., None]
    weight_two = lambdas.reshape(kv_heads, group, 1, 1)
    difference = ratio[:, :, 0] - weight_two * ratio[:, :, 1]
    att_rows = difference.transpose(2, 0, 1, 3).reshape(tok_rows, q_heads, 2 * HEAD_DIM)
    att_normed = (rms_scale(att_rows, head_gain) * (1.0 - LAMBDA_INIT)).astype(jnp.bfloat16)
    att_out = att_normed.reshape(tok_rows, q_heads * 2 * HEAD_DIM)
    glu_rows = (projected[3] * jax.nn.sigmoid(projected[4])).astype(jnp.bfloat16)
    padded = with_halo(glu_rows, (("sp", 0),), CONV_W // 2)
    conv_sum = jnp.zeros((tok_rows, glu_rows.shape[1]), jnp.float32)
    for offset in range(CONV_W):
        conv_sum = conv_sum + conv_weight[offset] * padded[offset : offset + tok_rows].astype(
            jnp.float32
        )
    squares = lax.psum(jnp.sum(conv_sum * conv_sum, axis=1), "tp")
    scaled = conv_sum * lax.rsqrt(squares / C_CH + EPS)[:, None] * channel_gain
    conv_out = jax.nn.silu(scaled).astype(jnp.bfloat16)
    pieces = (
        lax.all_gather(attn_out_weight, "sp", axis=0, tiled=True),
        lax.all_gather(conv_out_weight, "sp", axis=0, tiled=True),
    )
    partial_term = contract_last(att_out, pieces[0]) + contract_last(conv_out, pieces[1])
    return lax.psum_scatter(
        partial_term.astype(jnp.bfloat16), "tp", scatter_dimension=0, tiled=True
    )


PLANE = 4
RING = 4
LOG2E = 1.4426950408889634


def where_am_i():
    me = lax.axis_index("sp")
    core = lax.axis_index("tp")
    group = me // PLANE
    spot = me % PLANE
    along_y = spot // 2
    along_x = spot % 2
    base = group * PLANE
    x_peer = base + along_y * 2 + (1 - along_x)
    y_peer = base + (1 - along_y) * 2 + along_x
    diagonal = base + (1 - along_y) * 2 + (1 - along_x)
    line = [((group + hop) % RING) * PLANE + spot for hop in range(1, RING)]
    return core, group, spot, x_peer, y_peer, diagonal, line


def at(sp, tp):
    return {"sp": sp, "tp": tp}


def greet(peers):
    barrier = pltpu.get_barrier_semaphore()
    for peer in peers:
        pl.semaphore_signal(
            barrier, inc=1, device_id=peer, device_id_type=pl.DeviceIdType.MESH
        )
    pl.semaphore_wait(barrier, len(peers))


def send(src, dst, send_sem, recv_sem, peer):
    copy = pltpu.make_async_remote_copy(
        src_ref=src,
        dst_ref=dst,
        send_sem=send_sem,
        recv_sem=recv_sem,
        device_id=peer,
        device_id_type=pl.DeviceIdType.MESH,
    )
    copy.start()
    return copy


def gather_kernel(
    q_ref, k_ref, v_ref, g_ref, t_ref, wout, tout, own, ws, wr, xs, xr, us, ur, ds, dr, ps, pr
):
    core, group, spot, x_peer, y_peer, diagonal, line = where_am_i()
    other = 1 - core
    me = group * PLANE + spot
    greet(
        [at(chip, core) for chip in line]
        + [at(x_peer, core), at(y_peer, core), at(me, other)]
    )

    def segments(quarter):
        start = 0
        for ref in (q_ref, k_ref, v_ref, g_ref):
            if ref is g_ref:
                width = ref.shape[2]
                piece = ref.at[quarter]
            else:
                width = ref.shape[1] // RING
                piece = ref.at[:, pl.ds(pl.multiple_of(quarter * width, width), width)]
            yield piece, wout.at[group, spot, :, pl.ds(start, width)]
            start += width

    local_copies = [
        pltpu.make_async_copy(piece, place, own.at[i])
        for i, (piece, place) in enumerate(segments(group))
    ]
    local_copies.append(pltpu.make_async_copy(t_ref, tout.at[core, group], own.at[4]))
    for copy in local_copies:
        copy.start()
    first = []
    for hop, chip in enumerate(line):
        for i, (piece, place) in enumerate(segments(chip // PLANE)):
            first.append(
                send(piece, place, ws.at[hop * 4 + i], wr.at[hop * 4 + i], at(chip, core))
            )

    def token_copy(step, upward):
        move = 1 if upward else RING - 1
        source = (group + RING - step * move) % RING
        target = ((group + move) % RING) * PLANE + spot
        block = tout.at[core, source]
        sems = (us, ur) if upward else (ds, dr)
        return pltpu.make_async_remote_copy(
            src_ref=t_ref if step == 0 else block,
            dst_ref=block,
            send_sem=sems[0].at[step],
            recv_sem=sems[1].at[step],
            device_id=at(target, core),
            device_id_type=pl.DeviceIdType.MESH,
        )

    def partner_copy(hop):
        block = tout.at[core, (group + hop) % RING]
        return pltpu.make_async_remote_copy(
            src_ref=t_ref if hop == 0 else block,
            dst_ref=block,
            send_sem=ps.at[hop],
            recv_sem=pr.at[hop],
            device_id=at(me, other),
            device_id_type=pl.DeviceIdType.MESH,
        )

    def sends(step, upward):
        if upward:
            return jnp.logical_and(group >= step, group < RING - 1)
        return jnp.logical_and(group < RING - step, group > 0)

    def receives(step, upward):
        return group > step if upward else group < RING - 1 - step

    partner_copy(0).start()
    for upward in (True, False):

        @pl.when(sends(0, upward))
        def _():
            token_copy(0, upward).start()

    for copy in local_copies:
        copy.wait()
    for copy in first:
        copy.wait_recv()
    mine = wout.at[:, spot]
    ring = [
        send(mine, mine, xs.at[0], xr.at[0], at(x_peer, core)),
        send(mine, mine, xs.at[1], xr.at[1], at(y_peer, core)),
    ]
    for step in range(RING - 1):
        for upward in (True, False):

            @pl.when(receives(step, upward))
            def _():
                token_copy(step, upward).wait_recv()
                partner_copy(RING - 1 - step if upward else step + 1).start()

            if step < RING - 2:

                @pl.when(sends(step + 1, upward))
                def _():
                    token_copy(step + 1, upward).start()

    cut = RING // 2
    ring[0].wait_recv()
    piece = wout.at[pl.ds(0, cut), x_peer % PLANE]
    ring.append(send(piece, piece, xs.at[2], xr.at[2], at(y_peer, core)))
    ring[1].wait_recv()
    piece = wout.at[pl.ds(cut, cut), y_peer % PLANE]
    ring.append(send(piece, piece, xs.at[3], xr.at[3], at(x_peer, core)))
    for hop in range(RING):
        partner_copy(hop).wait()
    for step in range(RING - 1):
        for upward in (True, False):

            @pl.when(sends(step, upward))
            def _():
                token_copy(step, upward).wait_send()

    ring[2].wait_recv()
    ring[3].wait_recv()
    for copy in first + ring:
        copy.wait_send()


def squares_kernel(sq_ref, out_ref, own_sem, ss, sr):
    core, group, spot, x_peer, y_peer, diagonal, line = where_am_i()
    me = group * PLANE + spot
    other = 1 - core
    peers = [at(me, other)]
    for chip in line:
        peers.append(at(chip, core))
        peers.append(at(chip, other))
    greet(peers)
    mine = pltpu.make_async_copy(sq_ref, out_ref.at[group * 2 + core], own_sem.at[0])
    mine.start()
    copies = [
        send(sq_ref, out_ref.at[group * 2 + core], ss.at[i], sr.at[i], peer)
        for i, peer in enumerate(peers)
    ]
    mine.wait()
    for copy in copies:
        copy.wait()


def sum_kernel(p_ref, o_ref, near, mid, far, ns, nr, fs, fr):
    core, group, spot, x_peer, y_peer, diagonal, line = where_am_i()
    me = group * PLANE + spot
    other = 1 - core
    chips = [line[1], line[0], line[2], me]
    greet([at(me, other)] + [at(chip, core) for chip in chips[:3]])
    inner = [
        send(
            p_ref.at[chip // PLANE, other],
            near.at[slot],
            ns.at[slot],
            nr.at[slot],
            at(me, other),
        )
        for slot, chip in enumerate(chips)
    ]
    outer = []
    for slot, chip in enumerate(chips):
        inner[slot].wait_recv()
        total = p_ref[chip // PLANE, core].astype(jnp.float32) + near[slot].astype(jnp.float32)
        if slot < 3:
            mid[slot] = total.astype(jnp.bfloat16)
            outer.append(
                send(mid.at[slot], far.at[slot], fs.at[slot], fr.at[slot], at(chip, core))
            )
    for slot in range(3):
        outer[slot].wait_recv()
        total = total + far[slot].astype(jnp.float32)
    o_ref[...] = total.astype(o_ref.dtype)
    for copy in inner + outer:
        copy.wait_send()


def attend_kernel(
    lam_ref, gain_ref, q_ref, kv_ref, edge_ref, a_ref, c_ref,
    o_ref, edge_out, a_out, c_out,
    kv_all, numer, sums, own, es, er, zs, zr, ws, wr, xs, xr,
):
    core, group, spot, x_peer, y_peer, diagonal, line = where_am_i()
    greet(
        [at(x_peer, core), at(y_peer, core), at(diagonal, core)]
        + [at(chip, core) for chip in line]
    )
    keys = [
        send(kv_ref, kv_all.at[0], zs.at[0], zr.at[0], at(x_peer, core)),
        send(kv_ref, kv_all.at[1], zs.at[1], zr.at[1], at(y_peer, core)),
    ]
    base = group * PLANE
    after = base + (spot + 1) % PLANE
    before = base + (spot + PLANE - 1) % PLANE
    edges = [
        send(edge_ref.at[1], edge_out.at[0], es.at[0], er.at[0], at(after, core)),
        send(edge_ref.at[0], edge_out.at[1], es.at[1], er.at[1], at(before, core)),
    ]

    def columns(quarter):
        width = a_ref.shape[1] // RING
        return a_ref.at[:, pl.ds(pl.multiple_of(quarter * width, width), width)]

    mine = [
        pltpu.make_async_copy(columns(group), a_out.at[group, spot], own.at[0]),
        pltpu.make_async_copy(c_ref.at[group], c_out.at[group, spot], own.at[1]),
    ]
    for copy in mine:
        copy.start()
    first = []
    for hop, chip in enumerate(line):
        peer = at(chip, core)
        first.append(
            send(columns(chip // PLANE), a_out.at[group, spot], ws.at[hop], wr.at[hop], peer)
        )
        first.append(
            send(
                c_ref.at[chip // PLANE],
                c_out.at[group, spot],
                ws.at[3 + hop],
                wr.at[3 + hop],
                peer,
            )
        )

    width = 2 * HEAD_DIM
    rows = q_ref.shape[1]
    tall = rows // 2
    count = kv_ref.shape[0]
    step = 512

    def attend(block, fresh):
        @pl.loop(0, q_ref.shape[0] * 2)
        def _(turn):
            lead = turn // 2
            span = pl.ds(pl.multiple_of((turn % 2) * tall, tall), tall)
            query = q_ref[lead, span]
            if fresh:
                total = jnp.zeros((tall, width), jnp.float32)
                weighted = jnp.zeros((tall, width), jnp.float32)
            else:
                total = sums[lead, span]
                weighted = numer[lead, span]
            for start in range(0, count, step):
                stop = min(start + step, count)
                scores = contract_last(query, block[start:stop, :width])
                expo = jnp.exp2(scores * (LOG2E * HEAD_DIM ** (-0.5)))
                for lane in range(0, stop - start, width):
                    total = total + expo[:, lane : lane + width]
                weighted = weighted + jnp.dot(
                    expo.astype(jnp.bfloat16),
                    block[start:stop, width:],
                    preferred_element_type=jnp.float32,
                )
            sums[lead, span] = total
            numer[lead, span] = weighted

    attend(kv_ref, True)
    half = count // 2
    keys[0].wait_recv()
    keys.append(
        send(
            kv_all.at[0, pl.ds(0, half)],
            kv_all.at[2, pl.ds(0, half)],
            zs.at[2],
            zr.at[2],
            at(y_peer, core),
        )
    )
    keys[1].wait_recv()
    keys.append(
        send(
            kv_all.at[1, pl.ds(half, half)],
            kv_all.at[2, pl.ds(half, half)],
            zs.at[3],
            zr.at[3],
            at(x_peer, core),
        )
    )
    for copy in mine:
        copy.wait()
    for copy in first:
        copy.wait_recv()
    ring = []
    for i, buf in enumerate((a_out, c_out)):
        block = buf.at[:, spot]
        ring.append(send(block, block, xs.at[i], xr.at[i], at(x_peer, core)))
        ring.append(send(block, block, xs.at[2 + i], xr.at[2 + i], at(y_peer, core)))
    attend(kv_all.at[0], False)
    attend(kv_all.at[1], False)
    cut = RING // 2
    for i, buf in enumerate((a_out, c_out)):
        ring[2 * i].wait_recv()
        piece = buf.at[pl.ds(0, cut), x_peer % PLANE]
        ring.append(send(piece, piece, xs.at[4 + i], xr.at[4 + i], at(y_peer, core)))
        ring[2 * i + 1].wait_recv()
        piece = buf.at[pl.ds(cut, cut), y_peer % PLANE]
        ring.append(send(piece, piece, xs.at[6 + i], xr.at[6 + i], at(x_peer, core)))
    keys[2].wait_recv()
    keys[3].wait_recv()
    attend(kv_all.at[2], False)
    for head in range(q_ref.shape[0] // 2):

        @pl.loop(0, 2)
        def _(turn):
            span = pl.ds(pl.multiple_of(turn * tall, tall), tall)
            ratios = [
                numer[2 * head + pair, span]
                / jnp.sum(sums[2 * head + pair, span], axis=1, keepdims=True)
                for pair in range(2)
            ]
            att = ratios[0] - lam_ref[head] * ratios[1]
            att = rms_scale(att, gain_ref[...]) * (1.0 - LAMBDA_INIT)
            o_ref[span, head * width : (head + 1) * width] = att.astype(o_ref.dtype)

    for copy in ring[4:]:
        copy.wait_recv()
    for copy in edges:
        copy.wait()
    for copy in keys + first + ring:
        copy.wait_send()


VMEM = pl.BlockSpec(memory_space=pltpu.VMEM)
DMA = pltpu.SemaphoreType.DMA


def exchange(kernel, number, shapes, scratch, *operands, scalars=0):
    return pl.pallas_call(
        kernel,
        out_shape=shapes,
        in_specs=[pl.BlockSpec(memory_space=pltpu.SMEM)] * scalars
        + [VMEM] * (len(operands) - scalars),
        out_specs=jax.tree.map(lambda _: VMEM, shapes),
        scratch_shapes=scratch,
        compiler_params=pltpu.CompilerParams(
            collective_id=number, has_side_effects=True, vmem_limit_bytes=56 * 2**20
        ),
        name=kernel.__name__,
    )(*operands)


def grouped(
    tokens,
    norm_gain,
    query_weight,
    key_weight,
    value_weight,
    glu_value_weight,
    glu_gate_weight,
    query_gain,
    key_gain,
    lambdas,
    head_gain,
    conv_weight,
    channel_gain,
    attn_out_weight,
    conv_out_weight,
):
    bf16, f32 = jnp.bfloat16, jnp.float32
    shape = jax.ShapeDtypeStruct
    me = lax.axis_index("sp")
    group, spot = me // PLANE, me % PLANE
    depth = query_weight.shape[0]
    width = 2 * HEAD_DIM
    q_cols = query_weight.shape[1] // RING
    k_cols = key_weight.shape[1] // RING
    channels = glu_value_weight.shape[1] // RING
    q_heads = q_cols // width

    def quarters(*arrays):
        cut = [a.reshape(a.shape[0], RING, a.shape[1] // RING) for a in arrays]
        return jnp.concatenate(cut, axis=2).transpose(1, 0, 2)

    tok_rows, half_width = tokens.shape
    columns = q_cols + 2 * k_cols + 2 * channels
    w_all, t_all = exchange(
        gather_kernel,
        0,
        (
            shape((RING, PLANE, depth, columns), bf16),
            shape((2, RING, tok_rows, half_width), bf16),
        ),
        [DMA((5,)), DMA((12,)), DMA((12,)), DMA((4,)), DMA((4,))]
        + [DMA((3,))] * 4
        + [DMA((4,))] * 2,
        query_weight,
        key_weight,
        value_weight,
        quarters(glu_value_weight, glu_gate_weight),
        tokens,
    )
    w_all = w_all.reshape(RING * PLANE * depth, columns)
    rows = RING * tok_rows
    gathered = jnp.concatenate(
        [t_all[0].reshape(rows, half_width), t_all[1].reshape(rows, half_width)], axis=1
    ).astype(f32)
    normed = rms_scale(gathered, norm_gain).astype(bf16)
    qkv_cols = q_cols + 2 * k_cols
    qkv = jnp.dot(normed, w_all[:, :qkv_cols], preferred_element_type=f32)
    glu = jnp.dot(normed, w_all[:, qkv_cols:], preferred_element_type=f32)
    queries = qkv[:, :q_cols].reshape(rows, q_heads, 2, HEAD_DIM)
    queries = rms_scale(queries, query_gain).astype(bf16)
    low = jnp.pad(queries[:, :, 0], ((0, 0), (0, 0), (0, HEAD_DIM)))
    high = jnp.pad(queries[:, :, 1], ((0, 0), (0, 0), (HEAD_DIM, 0)))
    queries = jnp.stack([low, high], axis=0).transpose(2, 0, 1, 3)
    queries = queries.reshape(q_heads * 2, rows, width)
    keys = qkv[:, q_cols : q_cols + k_cols].reshape(rows, 2, HEAD_DIM)
    keys = rms_scale(keys, key_gain).astype(bf16).reshape(rows, width)
    kv = jnp.concatenate([keys, qkv[:, q_cols + k_cols :].astype(bf16)], axis=1)
    glu_rows = (glu[:, :channels] * jax.nn.sigmoid(glu[:, channels:])).astype(bf16)
    glu_rows = glu_rows.reshape(RING, tok_rows, channels)
    reach = CONV_W // 2
    border = 16
    edges = jnp.stack([glu_rows[:, :border], glu_rows[:, tok_rows - border :]])
    lam = lax.dynamic_slice_in_dim(lambdas, group * q_heads, q_heads, axis=0)
    att_out, halo, attn_all, conv_all = exchange(
        attend_kernel,
        1,
        (
            shape((rows, q_cols), bf16),
            shape(edges.shape, bf16),
            shape((RING, PLANE, depth, q_cols), bf16),
            shape((RING, PLANE, depth, channels), bf16),
        ),
        [
            pltpu.VMEM((3, rows, 2 * width), bf16),
            pltpu.VMEM((q_heads * 2, rows, width), f32),
            pltpu.VMEM((q_heads * 2, rows, width), f32),
            DMA((2,)),
            DMA((2,)),
            DMA((2,)),
            DMA((4,)),
            DMA((4,)),
            DMA((6,)),
            DMA((6,)),
            DMA((8,)),
            DMA((8,)),
        ],
        lam,
        head_gain.reshape(1, width),
        queries,
        kv,
        edges,
        attn_out_weight,
        quarters(conv_out_weight),
        scalars=1,
    )
    blank = jnp.zeros_like(halo[0, :1])
    tails = jnp.where(spot > 0, halo[0], jnp.concatenate([blank, halo[0, :-1]]))
    heads = jnp.where(spot < PLANE - 1, halo[1], jnp.concatenate([halo[1, 1:], blank]))
    padded = jnp.concatenate(
        [tails[:, border - reach :], glu_rows, heads[:, :reach]], axis=1
    ).astype(f32)
    taps = jnp.concatenate([conv_weight, channel_gain[None]], axis=0)
    taps = lax.dynamic_slice_in_dim(taps, group * channels, channels, axis=1)
    conv_sum = jnp.zeros((RING, tok_rows, channels), f32)
    for offset in range(CONV_W):
        conv_sum = conv_sum + taps[offset] * padded[:, offset : offset + tok_rows]
    conv_sum = conv_sum.reshape(rows, channels)
    squares = jnp.sum(conv_sum * conv_sum, axis=1).reshape(rows // 128, 128)
    squares = jnp.pad(squares, ((0, -squares.shape[0] % 8), (0, 0)))
    shared = exchange(
        squares_kernel,
        2,
        shape((2 * RING,) + squares.shape, f32),
        [DMA((1,)), DMA((7,)), DMA((7,))],
        squares,
    )
    squares = jnp.sum(shared, axis=0).reshape(-1)[:rows]
    scaled = conv_sum * lax.rsqrt(squares / C_CH + EPS)[:, None] * taps[CONV_W]
    conv_out = jax.nn.silu(scaled).astype(bf16)

    model = RING * PLANE * depth
    mixed = contract_last(att_out, attn_all.reshape(model, q_cols)) + contract_last(
        conv_out, conv_all.reshape(model, channels)
    )
    mixed = mixed.astype(bf16).reshape(RING, 2, tok_rows // 2, model)
    block = mixed.shape[2:]
    return exchange(
        sum_kernel,
        3,
        shape(block, bf16),
        [
            pltpu.VMEM((4,) + block, bf16),
            pltpu.VMEM((3,) + block, bf16),
            pltpu.VMEM((3,) + block, bf16),
            DMA((4,)),
            DMA((4,)),
            DMA((3,)),
            DMA((3,)),
        ],
        mixed,
    )


def body_for(mesh):
    if mesh.shape["sp"] == RING * PLANE and mesh.shape["tp"] == 2:
        return grouped
    return local


def solution(mesh):
    return jax.shard_map(
        body_for(mesh),
        mesh=mesh,
        in_specs=(
            P("sp", "tp"),
            P(),
            P("sp", "tp"),
            P("sp", "tp"),
            P("sp", "tp"),
            P("sp", "tp"),
            P("sp", "tp"),
            P(),
            P(),
            P("tp"),
            P(),
            P(None, "tp"),
            P("tp"),
            P("sp", "tp"),
            P("sp", "tp"),
        ),
        out_specs=P(("sp", "tp"), None),
        check_vma=False,
    )
```

```python
import jax
import jax.numpy as jnp
from jax import lax
from jax.experimental import pallas as pl
from jax.experimental.pallas import tpu as pltpu
from jax.sharding import PartitionSpec as P

HEAD_DIM = 64
C_CH = 1536
CONV_W = 31


EPS = 1e-06
LAMBDA_INIT = 0.2


def with_halo(cells, sides, width):
    for axis, dim in sides:
        count = lax.axis_size(axis)
        ends = count - 1
        head = lax.slice_in_dim(cells, 0, width, axis=dim)
        tail = lax.slice_in_dim(cells, cells.shape[dim] - width, cells.shape[dim], axis=dim)
        cells = jnp.concatenate(
            [
                lax.ppermute(tail, axis, [(i, (i + 1) % count) for i in range(ends)]),
                cells,
                lax.ppermute(head, axis, [((i + 1) % count, i) for i in range(ends)]),
            ],
            axis=dim,
        )
    return cells


def rms_scale(values, gain):
    return values * lax.rsqrt(jnp.mean(values * values, axis=-1, keepdims=True) + EPS) * gain


def contract_last(left, right):
    return lax.dot_general(
        left, right, (((1,), (1,)), ((), ())), preferred_element_type=jnp.float32
    )


def local(
    tokens,
    norm_gain,
    query_weight,
    key_weight,
    value_weight,
    glu_value_weight,
    glu_gate_weight,
    query_gain,
    key_gain,
    lambdas,
    head_gain,
    conv_weight,
    channel_gain,
    attn_out_weight,
    conv_out_weight,
):
    gathered = lax.all_gather(tokens, "tp", axis=1, tiled=True).astype(jnp.float32)
    normed = rms_scale(gathered, norm_gain).astype(jnp.bfloat16)
    tok_rows, model_width = normed.shape
    pieces = (
        lax.all_gather(query_weight, "sp", axis=0, tiled=True),
        lax.all_gather(key_weight, "sp", axis=0, tiled=True),
        lax.all_gather(value_weight, "sp", axis=0, tiled=True),
        lax.all_gather(glu_value_weight, "sp", axis=0, tiled=True),
        lax.all_gather(glu_gate_weight, "sp", axis=0, tiled=True),
    )
    projected = tuple(
        (jnp.dot(normed, w_piece, preferred_element_type=jnp.float32) for w_piece in pieces)
    )
    q_heads = query_weight.shape[1] // (2 * HEAD_DIM)
    kv_heads = key_weight.shape[1] // (2 * HEAD_DIM)
    group = q_heads // kv_heads
    queries = projected[0].reshape(tok_rows, q_heads, 2, HEAD_DIM)
    query_normed = rms_scale(queries, query_gain).astype(jnp.bfloat16)
    query_blocks = query_normed.reshape(tok_rows, kv_heads, group, 2, HEAD_DIM).transpose(
        1, 2, 3, 0, 4
    )
    keys = projected[1].reshape(tok_rows, kv_heads, 2, HEAD_DIM)
    key_rows = (
        rms_scale(keys, key_gain).astype(jnp.bfloat16).reshape(tok_rows, kv_heads * 2 * HEAD_DIM)
    )
    value_rows = projected[2].astype(jnp.bfloat16)

    def attend_block(carry, key_block, value_block):
        run_max, run_sum, numer = carry
        key_count = key_block.shape[0]
        key_heads = key_block.reshape(key_count, kv_heads, 2, HEAD_DIM).transpose(1, 2, 0, 3)
        value_heads = value_block.reshape(key_count, kv_heads, 2 * HEAD_DIM).transpose(1, 0, 2)
        scores = jnp.einsum(
            "kgprd,kpnd->kgprn", query_blocks, key_heads, preferred_element_type=jnp.float32
        ) * HEAD_DIM ** (-0.5)
        new_max = jnp.maximum(run_max, jnp.max(scores, axis=-1))
        expo = jnp.exp(scores - new_max[..., None])
        factor = jnp.exp(run_max - new_max)
        run_sum = run_sum * factor + jnp.sum(expo, axis=-1)
        numer = numer * factor[..., None] + jnp.einsum(
            "kgprn,knd->kgprd",
            expo.astype(jnp.bfloat16),
            value_heads,
            preferred_element_type=jnp.float32,
        )
        return (new_max, run_sum, numer)

    start_carry = (
        jnp.full((kv_heads, group, 2, tok_rows), -jnp.inf, jnp.float32),
        jnp.zeros((kv_heads, group, 2, tok_rows), jnp.float32),
        jnp.zeros((kv_heads, group, 2, tok_rows, 2 * HEAD_DIM), jnp.float32),
    )
    carry = start_carry
    pieces = (
        lax.all_gather(key_rows, "sp", axis=0, tiled=True),
        lax.all_gather(value_rows, "sp", axis=0, tiled=True),
    )
    key_count = pieces[0].shape[0]
    step_rows = key_count
    while step_rows > 1024 and step_rows % 2 == 0:
        step_rows = step_rows // 2
    turn_count = key_count // step_rows
    key_steps = pieces[0].reshape(turn_count, step_rows, pieces[0].shape[1])
    value_steps = pieces[1].reshape(turn_count, step_rows, pieces[1].shape[1])

    def one_turn(inner, both):
        return (attend_block(inner, both[0], both[1]), None)

    carry, unused = lax.scan(one_turn, carry, (key_steps, value_steps))
    run_max, run_sum, numer = carry
    ratio = numer / run_sum[..., None]
    weight_two = lambdas.reshape(kv_heads, group, 1, 1)
    difference = ratio[:, :, 0] - weight_two * ratio[:, :, 1]
    att_rows = difference.transpose(2, 0, 1, 3).reshape(tok_rows, q_heads, 2 * HEAD_DIM)
    att_normed = (rms_scale(att_rows, head_gain) * (1.0 - LAMBDA_INIT)).astype(jnp.bfloat16)
    att_out = att_normed.reshape(tok_rows, q_heads * 2 * HEAD_DIM)
    glu_rows = (projected[3] * jax.nn.sigmoid(projected[4])).astype(jnp.bfloat16)
    padded = with_halo(glu_rows, (("sp", 0),), CONV_W // 2)
    conv_sum = jnp.zeros((tok_rows, glu_rows.shape[1]), jnp.float32)
    for offset in range(CONV_W):
        conv_sum = conv_sum + conv_weight[offset] * padded[offset : offset + tok_rows].astype(
            jnp.float32
        )
    squares = lax.psum(jnp.sum(conv_sum * conv_sum, axis=1), "tp")
    scaled = conv_sum * lax.rsqrt(squares / C_CH + EPS)[:, None] * channel_gain
    conv_out = jax.nn.silu(scaled).astype(jnp.bfloat16)
    pieces = (
        lax.all_gather(attn_out_weight, "sp", axis=0, tiled=True),
        lax.all_gather(conv_out_weight, "sp", axis=0, tiled=True),
    )
    partial_term = contract_last(att_out, pieces[0]) + contract_last(conv_out, pieces[1])
    return lax.psum_scatter(
        partial_term.astype(jnp.bfloat16), "tp", scatter_dimension=0, tiled=True
    )


PLANE = 4
RING = 4
LOG2E = 1.4426950408889634


def where_am_i():
    me = lax.axis_index("sp")
    core = lax.axis_index("tp")
    group = me // PLANE
    spot = me % PLANE
    along_y = spot // 2
    along_x = spot % 2
    base = group * PLANE
    x_peer = base + along_y * 2 + (1 - along_x)
    y_peer = base + (1 - along_y) * 2 + along_x
    diagonal = base + (1 - along_y) * 2 + (1 - along_x)
    line = [((group + hop) % RING) * PLANE + spot for hop in range(1, RING)]
    return core, group, spot, x_peer, y_peer, diagonal, line


def at(sp, tp):
    return {"sp": sp, "tp": tp}


def greet(peers):
    barrier = pltpu.get_barrier_semaphore()
    for peer in peers:
        pl.semaphore_signal(
            barrier, inc=1, device_id=peer, device_id_type=pl.DeviceIdType.MESH
        )
    pl.semaphore_wait(barrier, len(peers))


def send(src, dst, send_sem, recv_sem, peer):
    copy = pltpu.make_async_remote_copy(
        src_ref=src,
        dst_ref=dst,
        send_sem=send_sem,
        recv_sem=recv_sem,
        device_id=peer,
        device_id_type=pl.DeviceIdType.MESH,
    )
    copy.start()
    return copy


def gather_kernel(
    q_ref, k_ref, v_ref, g_ref, t_ref, wout, tout, own, ws, wr, xs, xr, us, ur, ds, dr, ps, pr
):
    core, group, spot, x_peer, y_peer, diagonal, line = where_am_i()
    other = 1 - core
    me = group * PLANE + spot
    greet(
        [at(chip, core) for chip in line]
        + [at(x_peer, core), at(y_peer, core), at(me, other)]
    )

    def segments(quarter):
        start = 0
        for ref in (q_ref, k_ref, v_ref, g_ref):
            if ref is g_ref:
                width = ref.shape[2]
                piece = ref.at[quarter]
            else:
                width = ref.shape[1] // RING
                piece = ref.at[:, pl.ds(pl.multiple_of(quarter * width, width), width)]
            yield piece, wout.at[group, spot, :, pl.ds(start, width)]
            start += width

    local_copies = [
        pltpu.make_async_copy(piece, place, own.at[i])
        for i, (piece, place) in enumerate(segments(group))
    ]
    local_copies.append(pltpu.make_async_copy(t_ref, tout.at[core, group], own.at[4]))
    for copy in local_copies:
        copy.start()
    pieces = [list(segments(chip // PLANE)) for chip in line]
    first = []
    for i in range(4):
        for hop, chip in enumerate(line):
            piece, place = pieces[hop][i]
            first.append(
                send(piece, place, ws.at[hop * 4 + i], wr.at[hop * 4 + i], at(chip, core))
            )

    def token_copy(step, upward):
        move = 1 if upward else RING - 1
        source = (group + RING - step * move) % RING
        target = ((group + move) % RING) * PLANE + spot
        block = tout.at[core, source]
        sems = (us, ur) if upward else (ds, dr)
        return pltpu.make_async_remote_copy(
            src_ref=t_ref if step == 0 else block,
            dst_ref=block,
            send_sem=sems[0].at[step],
            recv_sem=sems[1].at[step],
            device_id=at(target, core),
            device_id_type=pl.DeviceIdType.MESH,
        )

    def partner_copy(hop):
        block = tout.at[core, (group + hop) % RING]
        return pltpu.make_async_remote_copy(
            src_ref=t_ref if hop == 0 else block,
            dst_ref=block,
            send_sem=ps.at[hop],
            recv_sem=pr.at[hop],
            device_id=at(me, other),
            device_id_type=pl.DeviceIdType.MESH,
        )

    def sends(step, upward):
        if upward:
            return jnp.logical_and(group >= step, group < RING - 1)
        return jnp.logical_and(group < RING - step, group > 0)

    def receives(step, upward):
        return group > step if upward else group < RING - 1 - step

    partner_copy(0).start()
    for upward in (True, False):

        @pl.when(sends(0, upward))
        def _():
            token_copy(0, upward).start()

    for copy in local_copies:
        copy.wait()
    edge = wout.shape[3] - g_ref.shape[2]
    parts = (pl.ds(0, edge), pl.ds(edge, g_ref.shape[2]))
    ring = []
    for part_no, arrivals in enumerate((first[:9], first[9:])):
        for copy in arrivals:
            copy.wait_recv()
        mine = wout.at[:, spot, :, parts[part_no]]
        sem = part_no * 4
        ring.append(send(mine, mine, xs.at[sem], xr.at[sem], at(x_peer, core)))
        ring.append(send(mine, mine, xs.at[sem + 1], xr.at[sem + 1], at(y_peer, core)))
    cut = RING // 2
    relays = []
    for step in range(RING - 1):
        if step < len(parts):
            sem = step * 4
            ring[2 * step].wait_recv()
            piece = wout.at[pl.ds(0, cut), x_peer % PLANE, :, parts[step]]
            relays.append(send(piece, piece, xs.at[sem + 2], xr.at[sem + 2], at(y_peer, core)))
            ring[2 * step + 1].wait_recv()
            piece = wout.at[pl.ds(cut, cut), y_peer % PLANE, :, parts[step]]
            relays.append(send(piece, piece, xs.at[sem + 3], xr.at[sem + 3], at(x_peer, core)))
        for upward in (True, False):

            @pl.when(receives(step, upward))
            def _():
                token_copy(step, upward).wait_recv()
                partner_copy(RING - 1 - step if upward else step + 1).start()

            if step < RING - 2:

                @pl.when(sends(step + 1, upward))
                def _():
                    token_copy(step + 1, upward).start()

    for hop in range(RING):
        partner_copy(hop).wait()
    for step in range(RING - 1):
        for upward in (True, False):

            @pl.when(sends(step, upward))
            def _():
                token_copy(step, upward).wait_send()

    for copy in relays:
        copy.wait_recv()
    for copy in first + ring + relays:
        copy.wait_send()


def squares_kernel(sq_ref, out_ref, own_sem, ss, sr):
    core, group, spot, x_peer, y_peer, diagonal, line = where_am_i()
    me = group * PLANE + spot
    other = 1 - core
    peers = [at(me, other)]
    for chip in line:
        peers.append(at(chip, core))
        peers.append(at(chip, other))
    greet(peers)
    mine = pltpu.make_async_copy(sq_ref, out_ref.at[group * 2 + core], own_sem.at[0])
    mine.start()
    copies = [
        send(sq_ref, out_ref.at[group * 2 + core], ss.at[i], sr.at[i], peer)
        for i, peer in enumerate(peers)
    ]
    mine.wait()
    for copy in copies:
        copy.wait()


def sum_kernel(p_ref, o_ref, near, mid, below, above, ns, nr, us, ur, ds, dr):
    core, group, spot, x_peer, y_peer, diagonal, line = where_am_i()
    me = group * PLANE + spot
    other = 1 - core
    greet([at(me, other)] + [at(chip, core) for chip in line])
    upper = (2 * group) // RING

    def inner(goal):
        return pltpu.make_async_remote_copy(
            src_ref=p_ref.at[goal, other],
            dst_ref=near.at[goal],
            send_sem=ns.at[goal],
            recv_sem=nr.at[goal],
            device_id=at(me, other),
            device_id_type=pl.DeviceIdType.MESH,
        )

    for turn in range(RING):
        inner(upper * turn + (1 - upper) * (RING - 1 - turn)).start()

    def hop(goal, upward):
        move = 1 if upward else RING - 1
        return pltpu.make_async_remote_copy(
            src_ref=mid.at[goal],
            dst_ref=(below if upward else above).at[goal],
            send_sem=(us if upward else ds).at[goal],
            recv_sem=(ur if upward else dr).at[goal],
            device_id=at(((group + move) % RING) * PLANE + spot, core),
            device_id_type=pl.DeviceIdType.MESH,
        )

    def own(goal):
        return p_ref[goal, core].astype(jnp.float32) + near[goal].astype(jnp.float32)

    def move_on(goal, upward):
        start = 0 if upward else RING - 1
        passes = group < goal if upward else group > goal
        came = below if upward else above

        @pl.when(jnp.logical_and(passes, group == start))
        def _():
            mid[goal] = own(goal).astype(jnp.bfloat16)
            hop(goal, upward).start()

        @pl.when(jnp.logical_and(passes, group != start))
        def _():
            hop(goal, upward).wait_recv()
            mid[goal] = (own(goal) + came[goal].astype(jnp.float32)).astype(jnp.bfloat16)
            hop(goal, upward).start()

    @pl.when(upper == 0)
    def _():
        for goal in range(RING - 1, -1, -1):
            inner(goal).wait_recv()
            if goal > 0:
                move_on(goal, True)
        for goal in range(RING // 2 - 1):
            move_on(goal, False)

    @pl.when(upper == 1)
    def _():
        for goal in range(RING):
            inner(goal).wait_recv()
            if goal < RING - 1:
                move_on(goal, False)
        for goal in range(RING - 1, RING // 2, -1):
            move_on(goal, True)

    for goal in range(RING):

        @pl.when(group == goal)
        def _():
            if goal > 0:
                hop(goal, True).wait_recv()
            if goal < RING - 1:
                hop(goal, False).wait_recv()
            total = own(goal)
            if goal > 0:
                total = total + below[goal].astype(jnp.float32)
            if goal < RING - 1:
                total = total + above[goal].astype(jnp.float32)
            o_ref[...] = total.astype(o_ref.dtype)

    for goal in range(RING):
        inner(goal).wait_send()

        @pl.when(group < goal)
        def _():
            hop(goal, True).wait_send()

        @pl.when(group > goal)
        def _():
            hop(goal, False).wait_send()


def attend_kernel(
    lam_ref, gain_ref, q_ref, kv_ref, edge_ref, a_ref, c_ref,
    o_ref, edge_out, a_out, c_out,
    kv_all, numer, sums, own, es, er, zs, zr, ws, wr, xs, xr,
):
    core, group, spot, x_peer, y_peer, diagonal, line = where_am_i()
    greet(
        [at(x_peer, core), at(y_peer, core), at(diagonal, core)]
        + [at(chip, core) for chip in line]
    )
    keys = [
        send(kv_ref, kv_all.at[0], zs.at[0], zr.at[0], at(x_peer, core)),
        send(kv_ref, kv_all.at[1], zs.at[1], zr.at[1], at(y_peer, core)),
    ]
    base = group * PLANE
    after = base + (spot + 1) % PLANE
    before = base + (spot + PLANE - 1) % PLANE
    edges = [
        send(edge_ref.at[1], edge_out.at[0], es.at[0], er.at[0], at(after, core)),
        send(edge_ref.at[0], edge_out.at[1], es.at[1], er.at[1], at(before, core)),
    ]

    def columns(quarter):
        width = a_ref.shape[1] // RING
        return a_ref.at[:, pl.ds(pl.multiple_of(quarter * width, width), width)]

    mine = [
        pltpu.make_async_copy(columns(group), a_out.at[group, spot], own.at[0]),
        pltpu.make_async_copy(c_ref.at[group], c_out.at[group, spot], own.at[1]),
    ]
    for copy in mine:
        copy.start()
    first = []
    for hop, chip in enumerate(line):
        peer = at(chip, core)
        first.append(
            send(columns(chip // PLANE), a_out.at[group, spot], ws.at[hop], wr.at[hop], peer)
        )
        first.append(
            send(
                c_ref.at[chip // PLANE],
                c_out.at[group, spot],
                ws.at[3 + hop],
                wr.at[3 + hop],
                peer,
            )
        )

    width = 2 * HEAD_DIM
    rows = q_ref.shape[1]
    tall = rows // 2
    count = kv_ref.shape[0]
    step = 512

    def attend(block, fresh):
        @pl.loop(0, q_ref.shape[0] * 2)
        def _(turn):
            lead = turn // 2
            span = pl.ds(pl.multiple_of((turn % 2) * tall, tall), tall)
            query = q_ref[lead, span]
            if fresh:
                total = jnp.zeros((tall, width), jnp.float32)
                weighted = jnp.zeros((tall, width), jnp.float32)
            else:
                total = sums[lead, span]
                weighted = numer[lead, span]
            for start in range(0, count, step):
                stop = min(start + step, count)
                scores = contract_last(query, block[start:stop, :width])
                expo = jnp.exp2(scores * (LOG2E * HEAD_DIM ** (-0.5)))
                for lane in range(0, stop - start, width):
                    total = total + expo[:, lane : lane + width]
                weighted = weighted + jnp.dot(
                    expo.astype(jnp.bfloat16),
                    block[start:stop, width:],
                    preferred_element_type=jnp.float32,
                )
            sums[lead, span] = total
            numer[lead, span] = weighted

    attend(kv_ref, True)
    half = count // 2
    keys[0].wait_recv()
    keys.append(
        send(
            kv_all.at[0, pl.ds(0, half)],
            kv_all.at[2, pl.ds(0, half)],
            zs.at[2],
            zr.at[2],
            at(y_peer, core),
        )
    )
    keys[1].wait_recv()
    keys.append(
        send(
            kv_all.at[1, pl.ds(half, half)],
            kv_all.at[2, pl.ds(half, half)],
            zs.at[3],
            zr.at[3],
            at(x_peer, core),
        )
    )
    for copy in mine:
        copy.wait()
    for copy in first:
        copy.wait_recv()
    ring = []
    for i, buf in enumerate((a_out, c_out)):
        block = buf.at[:, spot]
        ring.append(send(block, block, xs.at[i], xr.at[i], at(x_peer, core)))
        ring.append(send(block, block, xs.at[2 + i], xr.at[2 + i], at(y_peer, core)))
    attend(kv_all.at[0], False)
    attend(kv_all.at[1], False)
    keys[2].wait_recv()
    keys[3].wait_recv()
    attend(kv_all.at[2], False)
    cut = RING // 2
    for i, buf in enumerate((a_out, c_out)):
        ring[2 * i].wait_recv()
        piece = buf.at[pl.ds(0, cut), x_peer % PLANE]
        ring.append(send(piece, piece, xs.at[4 + i], xr.at[4 + i], at(y_peer, core)))
        ring[2 * i + 1].wait_recv()
        piece = buf.at[pl.ds(cut, cut), y_peer % PLANE]
        ring.append(send(piece, piece, xs.at[6 + i], xr.at[6 + i], at(x_peer, core)))
    for head in range(q_ref.shape[0] // 2):

        @pl.loop(0, 2)
        def _(turn):
            span = pl.ds(pl.multiple_of(turn * tall, tall), tall)
            ratios = [
                numer[2 * head + pair, span]
                / jnp.sum(sums[2 * head + pair, span], axis=1, keepdims=True)
                for pair in range(2)
            ]
            att = ratios[0] - lam_ref[group * (q_ref.shape[0] // 2) + head] * ratios[1]
            att = rms_scale(att, gain_ref[...]) * (1.0 - LAMBDA_INIT)
            o_ref[span, head * width : (head + 1) * width] = att.astype(o_ref.dtype)

    for copy in ring[4:]:
        copy.wait_recv()
    for copy in edges:
        copy.wait()
    for copy in keys + first + ring:
        copy.wait_send()


VMEM = pl.BlockSpec(memory_space=pltpu.VMEM)
DMA = pltpu.SemaphoreType.DMA


def exchange(kernel, number, shapes, scratch, *operands, scalars=0, far=()):
    return pl.pallas_call(
        kernel,
        out_shape=shapes,
        in_specs=[pl.BlockSpec(memory_space=pltpu.SMEM)] * scalars
        + [
            pl.BlockSpec(memory_space=pl.ANY) if i in far else VMEM
            for i in range(scalars, len(operands))
        ],
        out_specs=jax.tree.map(lambda _: VMEM, shapes),
        scratch_shapes=scratch,
        compiler_params=pltpu.CompilerParams(
            collective_id=number, has_side_effects=True, vmem_limit_bytes=56 * 2**20
        ),
        name=kernel.__name__,
    )(*operands)


def grouped(
    tokens,
    norm_gain,
    query_weight,
    key_weight,
    value_weight,
    glu_value_weight,
    glu_gate_weight,
    query_gain,
    key_gain,
    lambdas,
    head_gain,
    conv_weight,
    channel_gain,
    attn_out_weight,
    conv_out_weight,
):
    bf16, f32 = jnp.bfloat16, jnp.float32
    shape = jax.ShapeDtypeStruct
    me = lax.axis_index("sp")
    group, spot = me // PLANE, me % PLANE
    depth = query_weight.shape[0]
    width = 2 * HEAD_DIM
    q_cols = query_weight.shape[1] // RING
    k_cols = key_weight.shape[1] // RING
    channels = glu_value_weight.shape[1] // RING
    q_heads = q_cols // width

    def quarters(*arrays):
        cut = [a.reshape(a.shape[0], RING, a.shape[1] // RING) for a in arrays]
        return jnp.concatenate(cut, axis=2).transpose(1, 0, 2)

    tok_rows, half_width = tokens.shape
    columns = q_cols + 2 * k_cols + 2 * channels
    w_all, t_all = exchange(
        gather_kernel,
        0,
        (
            shape((RING, PLANE, depth, columns), bf16),
            shape((2, RING, tok_rows, half_width), bf16),
        ),
        [DMA((5,)), DMA((12,)), DMA((12,)), DMA((8,)), DMA((8,))]
        + [DMA((3,))] * 4
        + [DMA((4,))] * 2,
        query_weight,
        key_weight,
        value_weight,
        quarters(glu_value_weight, glu_gate_weight),
        tokens,
        far=(0, 1, 2, 4),
    )
    w_all = w_all.reshape(RING * PLANE * depth, columns)
    rows = RING * tok_rows
    gathered = jnp.concatenate(
        [t_all[0].reshape(rows, half_width), t_all[1].reshape(rows, half_width)], axis=1
    ).astype(f32)
    normed = rms_scale(gathered, norm_gain).astype(bf16)
    qkv_cols = q_cols + 2 * k_cols
    qkv = jnp.dot(normed, w_all[:, :qkv_cols], preferred_element_type=f32)
    glu = jnp.dot(normed, w_all[:, qkv_cols:], preferred_element_type=f32)
    queries = qkv[:, :q_cols].reshape(rows, q_heads, 2, HEAD_DIM)
    queries = rms_scale(queries, query_gain).astype(bf16)
    low = jnp.pad(queries[:, :, 0], ((0, 0), (0, 0), (0, HEAD_DIM)))
    high = jnp.pad(queries[:, :, 1], ((0, 0), (0, 0), (HEAD_DIM, 0)))
    queries = jnp.stack([low, high], axis=0).transpose(2, 0, 1, 3)
    queries = queries.reshape(q_heads * 2, rows, width)
    keys = qkv[:, q_cols : q_cols + k_cols].reshape(rows, 2, HEAD_DIM)
    keys = rms_scale(keys, key_gain).astype(bf16).reshape(rows, width)
    kv = jnp.concatenate([keys, qkv[:, q_cols + k_cols :].astype(bf16)], axis=1)
    glu_rows = (glu[:, :channels] * jax.nn.sigmoid(glu[:, channels:])).astype(bf16)
    glu_rows = glu_rows.reshape(RING, tok_rows, channels)
    reach = CONV_W // 2
    border = 16
    edges = jnp.stack([glu_rows[:, :border], glu_rows[:, tok_rows - border :]])
    att_out, halo, attn_all, conv_all = exchange(
        attend_kernel,
        1,
        (
            shape((rows, q_cols), bf16),
            shape(edges.shape, bf16),
            shape((RING, PLANE, depth, q_cols), bf16),
            shape((RING, PLANE, depth, channels), bf16),
        ),
        [
            pltpu.VMEM((3, rows, 2 * width), bf16),
            pltpu.VMEM((q_heads * 2, rows, width), f32),
            pltpu.VMEM((q_heads * 2, rows, width), f32),
            DMA((2,)),
            DMA((2,)),
            DMA((2,)),
            DMA((4,)),
            DMA((4,)),
            DMA((6,)),
            DMA((6,)),
            DMA((8,)),
            DMA((8,)),
        ],
        lambdas,
        head_gain.reshape(1, width),
        queries,
        kv,
        edges,
        attn_out_weight,
        quarters(conv_out_weight),
        scalars=1,
        far=(5,),
    )
    blank = jnp.zeros_like(halo[0, :1])
    tails = jnp.where(spot > 0, halo[0], jnp.concatenate([blank, halo[0, :-1]]))
    heads = jnp.where(spot < PLANE - 1, halo[1], jnp.concatenate([halo[1, 1:], blank]))
    padded = jnp.concatenate(
        [tails[:, border - reach :], glu_rows, heads[:, :reach]], axis=1
    ).astype(f32)
    taps = jnp.concatenate([conv_weight, channel_gain[None]], axis=0)
    taps = lax.dynamic_slice_in_dim(taps, group * channels, channels, axis=1)
    conv_sum = jnp.zeros((RING, tok_rows, channels), f32)
    for offset in range(CONV_W):
        conv_sum = conv_sum + taps[offset] * padded[:, offset : offset + tok_rows]
    conv_sum = conv_sum.reshape(rows, channels)
    squares = jnp.sum(conv_sum * conv_sum, axis=1).reshape(rows // 128, 128)
    squares = jnp.pad(squares, ((0, -squares.shape[0] % 8), (0, 0)))
    shared = exchange(
        squares_kernel,
        2,
        shape((2 * RING,) + squares.shape, f32),
        [DMA((1,)), DMA((7,)), DMA((7,))],
        squares,
    )
    squares = jnp.sum(shared, axis=0).reshape(-1)[:rows]
    scaled = conv_sum * lax.rsqrt(squares / C_CH + EPS)[:, None] * taps[CONV_W]
    conv_out = jax.nn.silu(scaled).astype(bf16)

    model = RING * PLANE * depth
    mixed = contract_last(att_out, attn_all.reshape(model, q_cols)) + contract_last(
        conv_out, conv_all.reshape(model, channels)
    )
    mixed = mixed.astype(bf16).reshape(RING, 2, tok_rows // 2, model)
    block = mixed.shape[2:]
    return exchange(
        sum_kernel,
        3,
        shape(block, bf16),
        [pltpu.VMEM((RING,) + block, bf16)] * 4 + [DMA((RING,))] * 6,
        mixed,
    )


def body_for(mesh):
    if mesh.shape["sp"] == RING * PLANE and mesh.shape["tp"] == 2:
        return grouped
    return local


def solution(mesh):
    return jax.shard_map(
        body_for(mesh),
        mesh=mesh,
        in_specs=(
            P("sp", "tp"),
            P(),
            P("sp", "tp"),
            P("sp", "tp"),
            P("sp", "tp"),
            P("sp", "tp"),
            P("sp", "tp"),
            P(),
            P(),
            P("tp"),
            P(),
            P(None, "tp"),
            P("tp"),
            P("sp", "tp"),
            P("sp", "tp"),
        ),
        out_specs=P(("sp", "tp"), None),
        check_vma=False,
    )
```
